256 devices in a mesh: kv: 16 (over y, x), tp: 16 (over z, core).
Axes of the slice: x: 4, y: 4, z: 8, core: 2. Of those that a mesh axis runs over, the one named last changes fastest.
Arguments:
- tokens: bfloat16 [16, 2048], P(None, 'kv'), may hold values from -40 to 40
- lengths: int32 [16], replicated, may hold values from 1 to 16384, 77824 in all
- cache_keys: bfloat16 [16, 16384, 16, 128], P(None, 'kv', 'tp'), may hold values from -200 to 200
- cache_values: bfloat16 [16, 16384, 16, 128], P(None, 'kv', 'tp'), may hold values from -6 to 6
- lambdas: float32 [16], P('tp'), may hold values from 0.3 to 0.8
- head_gain: bfloat16 [128], replicated, may hold values from 0.099609375 to 1.8984375
- attn_gain: bfloat16 [2048], P('kv'), may hold values from 0.099609375 to 1.8984375
- w_query: bfloat16 [2048, 2048], P('kv', 'tp'), may hold values from -0.125 to 0.125
- w_key: bfloat16 [2048, 2048], P('kv', 'tp'), may hold values from -0.5 to 0.5
- w_value: bfloat16 [2048, 2048], P('kv', 'tp'), may hold values from -0.125 to 0.125
- w_out: bfloat16 [2048, 2048], P('tp', 'kv'), may hold values from -0.125 to 0.125
- first_gain: bfloat16 [2048], P('kv'), may hold values from 0.099609375 to 1.8984375
- first_gate: bfloat16 [2048, 5632], P('kv', 'tp'), may hold values from -0.125 to 0.125
- first_up: bfloat16 [2048, 5632], P('kv', 'tp'), may hold values from -0.125 to 0.125
- first_down: bfloat16 [5632, 2048], P('tp', 'kv'), may hold values from -0.078125 to 0.078125
- second_gain: bfloat16 [2048], P('kv'), may hold values from 0.099609375 to 1.8984375
- second_gate: bfloat16 [2048, 5632], P('kv', 'tp'), may hold values from -0.125 to 0.125
- second_up: bfloat16 [2048, 5632], P('kv', 'tp'), may hold values from -0.125 to 0.125
- second_down: bfloat16 [5632, 2048], P('tp', 'kv'), may hold values from -0.078125 to 0.078125
Outputs:
- stream_out: bfloat16 [16, 2048], P(None, 'kv')
The draws below stay inside these ranges and needn't reach their ends.
Inputs may be any that keep to these rules, and one draw needn't show every extreme that they name: `lengths`: one sequence has exactly 16384 live positions.
All inputs are finite; a program needn't handle non-finite values.
Results may differ from the reference program's by a relative error of at most 0.02.
Values may be sent and summed in bfloat16 or wider, within the bound.
No kernel may reach another device: no remote copies, remote signals or barrier semaphores. Data moves between devices by JAX's collectives and lax.ppermute only.
A program may use at most 64 MiB of HBM per device.

```python
import math
import jax
import jax.numpy as jnp
import numpy as np
from jax import lax

D = 2048
FF = 5632
HEADS = 16
DK = 64
DV = 128
SEQS = 16
LENGTH = 16384


def draw_tokens(key, part):
    columns = jnp.arange(D, dtype=jnp.float32) / D
    col_scale = 0.5 * jnp.exp(math.log(4.0) * columns)[None, :]
    base = jnp.clip(jax.random.normal(key, (SEQS, D), jnp.float32), -6.0, 6.0)
    return (base * col_scale).astype(jnp.bfloat16)


def draw_cache_keys(key, part):
    shape_all = (SEQS, LENGTH, HEADS, 2 * DK)
    base = jnp.clip(jax.random.normal(key, shape_all, jnp.float32) * 1.75, -10.0, 10.0)
    return base.astype(jnp.bfloat16)


def steps_of(stream_key, dims, shards, low, largest):
    level = 1.0
    for dim, shards_of in shards:
        draws = jax.random.uniform(jax.random.fold_in(jax.random.fold_in(stream_key, 6), dim), (shards_of,), jnp.float32, low / len(shards), largest / len(shards))
        level = level * jnp.repeat(jnp.exp(draws), dims[dim] // shards_of).reshape((-1,) + (1,) * (len(dims) - 1 - dim))
    return level


def profile(number_of, total, reach, skew):
    portions = [(1 << 20) // math.isqrt(rank ** skew) + 1 for rank in range(2, number_of + 1)]
    surplus, counts = total - reach - (number_of - 1), [1] * (number_of - 1)
    while surplus > 0:
        candidates = [i for i in range(number_of - 1) if counts[i] < reach]
        pool, left = sum([portions[i] for i in candidates]), surplus
        for i in candidates:
            more = min(reach - counts[i], max(1, left * portions[i] // pool), surplus)
            counts[i] = counts[i] + more
            surplus = surplus - more
    return np.array([reach] + counts)


def uneven_parts(own_key, number_of, total, most, slope):
    if number_of == 2:
        one = jax.random.randint(own_key, (), max(1, total - most), min(most, total - 1) + 1)
        return jnp.stack([one, total - one])
    tallies = jnp.asarray(profile(number_of, total, most, slope), jnp.int32)
    pairs = (number_of - 1) // 2
    giver, sink = tallies[1:1 + 2 * pairs:2], tallies[2:2 + 2 * pairs:2]
    slack = jnp.minimum(giver - 1, most - sink)
    moved = jax.random.randint(jax.random.fold_in(own_key, 1), (pairs,), 0, 1 << 20) % (slack + 1)
    tallies = tallies.at[1:1 + 2 * pairs:2].set(giver - moved).at[2:2 + 2 * pairs:2].set(sink + moved)
    return tallies[jax.random.permutation(jax.random.fold_in(own_key, 2), number_of)]


def gaussian(own_key, extent, spread, limit, cuts=(), kind=jnp.bfloat16):
    entries = jax.random.normal(own_key, extent, jnp.float32) * spread
    if len(cuts) > 0:
        entries = steps_of(own_key, extent, cuts, -0.22, 0.18) * entries
    return jnp.clip(entries, min=-limit, max=limit).astype(kind)


def setup_inputs(seed: int = 0) -> dict:
    arg_keys = jax.random.split(jax.random.key(seed), 20)
    tokens = draw_tokens(jax.random.fold_in(arg_keys[19], 71), 0)
    lengths = uneven_parts(arg_keys[1], SEQS, LENGTH + (SEQS - 1) * (LENGTH // 4), LENGTH, 2).astype(jnp.int32)
    cache_keys = draw_cache_keys(jax.random.fold_in(arg_keys[19], 71), 0)
    cache_values = gaussian(arg_keys[3], (SEQS, LENGTH, HEADS, DV), 1.0, 6.0, ((1, 16), (2, 16)))
    lambdas = jnp.clip(0.3 + 0.5 * jax.random.uniform(arg_keys[4], (HEADS,), jnp.float32) ** steps_of(arg_keys[4], (HEADS,), ((0, 16),), -0.2, 0.2), 0.3, 0.8)
    head_gain = jnp.clip(1.0 + 0.18 * jax.random.normal(arg_keys[5], (DV,), jnp.float32), 0.099609375, 1.8984375).astype(jnp.bfloat16)
    attn_gain = jnp.clip(1.0 + 0.18 * jax.random.normal(arg_keys[6], (D,), jnp.float32), 0.099609375, 1.8984375).astype(jnp.bfloat16)
    w_query = gaussian(arg_keys[7], (D, HEADS * 2 * DK), D ** -0.5, 0.125, ((0, 16), (1, 16)))
    w_key = gaussian(arg_keys[8], (D, HEADS * 2 * DK), (D // 16) ** -0.5, 0.5, ((0, 16), (1, 16)))
    w_value = gaussian(arg_keys[9], (D, HEADS * DV), D ** -0.5, 0.125, ((0, 16), (1, 16)))
    w_out = gaussian(arg_keys[10], (HEADS * DV, D), (HEADS * DV) ** -0.5, 0.125, ((0, 16), (1, 16)))
    first_gain = jnp.clip(1.0 + 0.18 * jax.random.normal(arg_keys[11], (D,), jnp.float32), 0.099609375, 1.8984375).astype(jnp.bfloat16)
    first_gate = gaussian(arg_keys[12], (D, FF), D ** -0.5, 0.125, ((0, 16), (1, 16)))
    first_up = gaussian(arg_keys[13], (D, FF), D ** -0.5, 0.125, ((0, 16), (1, 16)))
    first_down = gaussian(arg_keys[14], (FF, D), FF ** -0.5, 0.078125, ((0, 16), (1, 16)))
    second_gain = jnp.clip(1.0 + 0.18 * jax.random.normal(arg_keys[15], (D,), jnp.float32), 0.099609375, 1.8984375).astype(jnp.bfloat16)
    second_gate = gaussian(arg_keys[16], (D, FF), D ** -0.5, 0.125, ((0, 16), (1, 16)))
    second_up = gaussian(arg_keys[17], (D, FF), D ** -0.5, 0.125, ((0, 16), (1, 16)))
    second_down = gaussian(arg_keys[18], (FF, D), FF ** -0.5, 0.078125, ((0, 16), (1, 16)))
    return {"tokens": tokens, "lengths": lengths, "cache_keys": cache_keys, "cache_values": cache_values, "lambdas": lambdas, "head_gain": head_gain, "attn_gain": attn_gain, "w_query": w_query, "w_key": w_key, "w_value": w_value, "w_out": w_out, "first_gain": first_gain, "first_gate": first_gate, "first_up": first_up, "first_down": first_down, "second_gain": second_gain, "second_gate": second_gate, "second_up": second_up, "second_down": second_down}


EPSILON = 1e-06
ROTARY_BASE = 10000.0
OUTPUT_KEEP = 0.8

def rotate(vectors, positions):
    half_width = vectors.shape[-1] // 2
    inv_freq = jnp.power(ROTARY_BASE, -jnp.arange(half_width, dtype=jnp.float32) / half_width)
    angles = positions.astype(jnp.float32)[:, None] * inv_freq[None, :]
    bcast_shape = (angles.shape[0],) + (1,) * (vectors.ndim - 2) + (half_width,)
    cosine = jnp.cos(angles).reshape(bcast_shape)
    sine_part = jnp.sin(angles).reshape(bcast_shape)
    first_half = vectors[..., :half_width]
    second_half = vectors[..., half_width:]
    return jnp.concatenate([first_half * cosine - second_half * sine_part, second_half * cosine + first_half * sine_part], axis=-1)

def channel_mix(stream, gain, w_gate, w_up, w_down):
    stream_f = stream.astype(jnp.float32)
    scaled = (stream_f * gain.astype(jnp.float32)).astype(jnp.bfloat16)
    row_scale = lax.rsqrt(lax.optimization_barrier(jnp.mean(stream_f * stream_f, axis=1, keepdims=True)) + EPSILON)
    gate = row_scale * jnp.dot(scaled, w_gate, preferred_element_type=jnp.float32)
    up_val = row_scale * jnp.dot(scaled, w_up, preferred_element_type=jnp.float32)
    hidden = (jax.nn.silu(gate) * up_val).astype(jnp.bfloat16)
    return (stream_f + 0.5 * jnp.dot(hidden, w_down, preferred_element_type=jnp.float32)).astype(jnp.bfloat16)

def reference(tokens, lengths, cache_keys, cache_values, lambdas, head_gain, attn_gain, w_query, w_key, w_value, w_out, first_gain, first_gate, first_up, first_down, second_gain, second_gate, second_up, second_down):
    first = channel_mix(tokens, first_gain, first_gate, first_up, first_down)
    seq_count = first.shape[0]
    stream_f = first.astype(jnp.float32)
    scaled = (stream_f * attn_gain.astype(jnp.float32)).astype(jnp.bfloat16)
    row_scale = lax.rsqrt(lax.optimization_barrier(jnp.mean(stream_f * stream_f, axis=1, keepdims=True)) + EPSILON)
    query = row_scale * jnp.dot(scaled, w_query, preferred_element_type=jnp.float32)
    key_new = row_scale * jnp.dot(scaled, w_key, preferred_element_type=jnp.float32)
    value_new = (row_scale * jnp.dot(scaled, w_value, preferred_element_type=jnp.float32)).astype(jnp.bfloat16)
    query = rotate(query.reshape(seq_count, HEADS, 2, DK), lengths).astype(jnp.bfloat16)
    key_new = rotate(key_new.reshape(seq_count, HEADS, 2, DK), lengths).astype(jnp.bfloat16)
    value_new = value_new.reshape(seq_count, HEADS, DV)
    live_mask = jnp.arange(LENGTH, dtype=jnp.int32)[None, :] < lengths[:, None]
    scale_att = DK ** (-0.5)

    def one_head(inputs):
        index, lam_value = inputs
        key_rows = lax.dynamic_index_in_dim(cache_keys, index, axis=2, keepdims=False).reshape(seq_count, LENGTH, 2, DK).astype(jnp.float32)
        value_rows = lax.dynamic_index_in_dim(cache_values, index, axis=2, keepdims=False).astype(jnp.float32)
        query_h = lax.dynamic_index_in_dim(query, index, axis=1, keepdims=False).astype(jnp.float32)
        key_h = lax.dynamic_index_in_dim(key_new, index, axis=1, keepdims=False).astype(jnp.float32)
        value_h = lax.dynamic_index_in_dim(value_new, index, axis=1, keepdims=False).astype(jnp.float32)
        scores = jnp.einsum('bcd,blcd->bcl', query_h, key_rows, precision=lax.Precision.HIGHEST) * scale_att
        scores = jnp.where(live_mask[:, None, :], scores, -jnp.inf)
        own_score = lax.optimization_barrier(jnp.sum(query_h * key_h, axis=2)) * scale_att
        peak_max = jnp.maximum(lax.optimization_barrier(jnp.max(scores, axis=2)), own_score)
        weights = jnp.exp(scores - peak_max[..., None])
        fresh_weight = jnp.exp(own_score - peak_max)
        denominator = lax.optimization_barrier(jnp.sum(weights, axis=2)) + fresh_weight
        rounded = lax.optimization_barrier(weights.astype(jnp.bfloat16)).astype(jnp.float32)
        summed = jnp.einsum('bcl,bld->bcd', rounded, value_rows, precision=lax.Precision.HIGHEST) + fresh_weight[..., None] * value_h[:, None, :]
        mixed = summed / denominator[..., None]
        return mixed[:, 0] - lam_value * mixed[:, 1]
    heads_out = lax.map(one_head, (jnp.arange(HEADS, dtype=jnp.int32), lambdas))
    heads_out = jnp.moveaxis(heads_out, 0, 1)
    norm_scale = lax.rsqrt(lax.optimization_barrier(jnp.mean(heads_out * heads_out, axis=2, keepdims=True)) + EPSILON)
    normed = (heads_out * norm_scale * head_gain.astype(jnp.float32) * OUTPUT_KEEP).astype(jnp.bfloat16)
    normed = normed.reshape(seq_count, HEADS * DV)
    second = (stream_f + jnp.dot(normed, w_out, preferred_element_type=jnp.float32)).astype(jnp.bfloat16)
    return channel_mix(second, second_gain, second_gate, second_up, second_down)
```

```python
import functools
import math

import jax
import jax.numpy as jnp
from jax import lax
from jax.experimental import pallas as pl
from jax.experimental.pallas import tpu as pltpu
from jax.sharding import Mesh
from jax.sharding import PartitionSpec as P

D = 2048
DK = 64
DV = 128
SEQS = 16
KV = ("kv_0", "kv_1")
EPSILON = 1e-06
ROTARY_BASE = 10000.0
OUTPUT_KEEP = 0.8
MASKED_SCORE = -1e30
F32 = jnp.float32
BF16 = jnp.bfloat16


def exchange(copies, axis):
    return lax.all_to_all(copies, axis, split_axis=0, concat_axis=0, tiled=True)


def cost(micros):
    return pl.CostEstimate(flops=int(micros * 5e8), bytes_accessed=1 << 16, transcendentals=0)


def local_call(body, outs, *arrays, scratch=(), smem=()):
    specs = [
        pl.BlockSpec(memory_space=pltpu.SMEM if i in smem else pltpu.VMEM)
        for i in range(len(arrays))
    ]
    return pl.pallas_call(
        body,
        out_shape=outs,
        in_specs=specs,
        out_specs=jax.tree.map(lambda _: pl.BlockSpec(memory_space=pltpu.VMEM), outs),
        scratch_shapes=list(scratch),
        compiler_params=pltpu.CompilerParams(vmem_limit_bytes=4 << 20),
        cost_estimate=cost(10),
    )(*arrays)


def dot_rows(a, b):
    return lax.dot_general(a, b, (((1,), (1,)), ((), ())), preferred_element_type=F32)


def dot(a, b):
    return jnp.dot(a, b, preferred_element_type=F32)


def put_copies(out_ref, at, value):
    for j in range(out_ref.shape[0]):
        out_ref[j, :, at : at + value.shape[1]] = value


def pieces(value, count):
    parts = []
    for _ in range(count):
        part = value.astype(BF16)
        parts.append(part)
        value = value - part.astype(F32)
    return parts


def with_columns(width, columns):
    lane = lax.broadcasted_iota(jnp.int32, (columns[0].shape[0], width), 1)
    out = jnp.zeros(lane.shape, F32)
    for i, c in enumerate(columns):
        out = jnp.where(lane == i, c.astype(F32), out)
    return out.astype(BF16)


def total(ref):
    out = ref[0].astype(F32)
    for j in range(1, ref.shape[0]):
        out = out + ref[j].astype(F32)
    return out


def gate_up_products(stream_f, gain_ref, gate_ref, up_ref, out_ref):
    scaled = (stream_f * gain_ref[...].astype(F32)).astype(BF16)
    square = jnp.sum(stream_f * stream_f, axis=1, keepdims=True)
    gate = dot_rows(scaled, gate_ref[...]).astype(BF16)
    up = dot_rows(scaled, up_ref[...]).astype(BF16)
    put_copies(out_ref, 0, gate)
    put_copies(out_ref, 352, with_columns(32, pieces(square, 2)))
    put_copies(out_ref, 384, up)
    put_copies(out_ref, 736, jnp.zeros((SEQS, 32), BF16))


def first_products(
    tokens_ref, gain_ref, gate_ref, up_ref, lambda_ref, out_ref, lambda_out, tokens, gain, gate, up,
    lam, sems
):
    copies = [
        pltpu.make_async_copy(src, dst, sems.at[i])
        for i, (src, dst) in enumerate(
            (
                (gate_ref, gate), (up_ref, up), (tokens_ref, tokens), (gain_ref, gain),
                (lambda_ref, lam),
            )
        )
    ]
    for copy in copies:
        copy.start()
    for copy in copies:
        copy.wait()
    gate_up_products(tokens[...].astype(F32), gain, gate, up, out_ref)
    lambda_out[...] = jnp.full(lambda_out.shape, lam[0], F32)


def second_products(stream_ref, got_ref, gain_ref, gate_ref, up_ref, out_ref, second_ref):
    second = (stream_ref[...].astype(F32) + total(got_ref)).astype(BF16)
    second_ref[...] = second
    gate_up_products(second.astype(F32), gain_ref, gate_ref, up_ref, out_ref)


def down_products(got_ref, down_ref, out_ref):
    summed = total(got_ref)
    square = summed[:, 352:353] + summed[:, 353:354]
    row_scale = lax.rsqrt(square / D + EPSILON)
    gate = row_scale * summed[:, :352]
    up = row_scale * summed[:, 384:736]
    hidden = (gate / (1.0 + jnp.exp(-gate)) * up).astype(BF16)
    put_copies(out_ref, 0, dot(hidden, down_ref[...]).astype(BF16))


def head_products(tokens_ref, got_ref, gain_ref, wq_ref, wk_ref, wv_ref, out_ref, first_ref):
    first = (tokens_ref[...].astype(F32) + 0.5 * total(got_ref)).astype(BF16)
    first_ref[...] = first
    stream_f = first.astype(F32)
    scaled = (stream_f * gain_ref[...].astype(F32)).astype(BF16)
    square = jnp.sum(stream_f * stream_f, axis=1, keepdims=True)
    query = dot(scaled, wq_ref[...]).astype(BF16)
    key = dot(scaled, wk_ref[...])
    value = dot(scaled, wv_ref[...])
    diagonal = lax.broadcasted_iota(jnp.int32, (SEQS, 128), 0) == lax.broadcasted_iota(
        jnp.int32, (SEQS, 128), 1
    )
    high, rest = pieces(jnp.sum(jnp.where(diagonal, square, 0.0), axis=0, keepdims=True), 2)
    row = lax.broadcasted_iota(jnp.int32, (8, 128), 0)
    squares = jnp.where(row == 2, high.astype(F32), jnp.where(row == 3, rest.astype(F32), 0.0))
    for j in range(SEQS):
        out_ref[j, :SEQS, :] = query
        tail = jnp.where(row == 0, key[j : j + 1], jnp.where(row == 1, value[j : j + 1], squares))
        out_ref[j, SEQS:, :] = tail.astype(BF16)


def rotary_tables(lengths_ref, rows, width):
    lane = lax.broadcasted_iota(jnp.int32, (rows, width), 1)
    row = lax.broadcasted_iota(jnp.int32, (rows, width), 0)
    place = jnp.zeros((rows, width), jnp.int32)
    for b in range(rows):
        place = jnp.where(row == b, lengths_ref[b], place)
    half = DK // 2
    step = (lane % half).astype(F32)
    angles = place.astype(F32) * jnp.exp(step * (-math.log(ROTARY_BASE) / half))
    low = (lane // half) % 2 == 0
    sine = jnp.sin(angles)
    return jnp.cos(angles), jnp.where(low, -sine, sine), low, lane


def attention(lengths_ref, got_ref, keys_ref, values_ref, out_ref):
    summed = total(got_ref)
    cosine, sine, low, lane = rotary_tables(lengths_ref, SEQS, 2 * DK)
    row = lax.broadcasted_iota(jnp.int32, lane.shape, 0)
    kv_index = lax.axis_index(KV)
    mine = row == kv_index
    square = jnp.sum(
        jnp.where(row == lane, summed[18:19] + summed[19:20], 0.0), axis=1, keepdims=True
    )
    row_scale = lax.rsqrt(square / D + EPSILON)

    def of_mine(x):
        return jnp.sum(jnp.where(mine, x, 0.0), axis=0, keepdims=True)

    def rotate(x, cosine, sine, low):
        swapped = jnp.where(low, pltpu.roll(x, 96, 1), pltpu.roll(x, 32, 1))
        return (x * cosine + swapped * sine).astype(BF16).astype(F32)

    def eight(x):
        return jnp.broadcast_to(x, (8, x.shape[1]))

    query = rotate(row_scale * summed[:SEQS], cosine, sine, low)
    my_scale = of_mine(jnp.broadcast_to(row_scale, lane.shape))
    key_new = rotate(
        eight(my_scale * summed[16:17]), eight(of_mine(cosine)), eight(of_mine(sine)), low[:8]
    )[:1]
    value_new = (my_scale * summed[17:18]).astype(BF16).astype(F32)
    scale_att = DK ** (-0.5)
    first_part = lane < DK
    both = jnp.concatenate(
        [jnp.where(first_part, query, 0.0), jnp.where(first_part, 0.0, query)], axis=0
    )
    rows = 2 * SEQS
    positions = keys_ref.shape[1]
    of_row = lax.broadcasted_iota(jnp.int32, (rows, DV), 0) % SEQS
    limit = jnp.zeros((rows, 1), jnp.int32)
    s = jnp.zeros((rows, positions), F32)
    for b in range(SEQS):
        picked = jnp.where(of_row == b, both, 0.0).astype(BF16)
        s = s + dot_rows(picked, keys_ref[b])
        limit = jnp.where(of_row[:, :1] == b, lengths_ref[b] - kv_index * positions, limit)
    alive = lax.broadcasted_iota(jnp.int32, (rows, positions), 1) < limit
    s = jnp.where(alive, s * scale_att, MASKED_SCORE)
    old = jnp.max(s, axis=1, keepdims=True)
    e = jnp.where(alive, jnp.exp(s - old), 0.0)
    l = jnp.sum(e, axis=1, keepdims=True)
    weights = e.astype(BF16)
    o = jnp.zeros((rows, DV), F32)
    for b in range(SEQS):
        o = jnp.where(of_row == b, dot(weights, values_ref[b]), o)
    here = of_row[:, :1] == kv_index
    own_score = scale_att * jnp.sum(both * key_new, axis=1, keepdims=True)
    own_score = jnp.where(here, own_score, MASKED_SCORE)
    peak = jnp.maximum(old, own_score)
    old_scale = jnp.exp(old - peak)
    fresh = jnp.where(here, jnp.exp(own_score - peak), 0.0)
    l = l * old_scale + fresh
    o = (o * old_scale + fresh * value_new).astype(BF16)
    lane = lane[:8]
    stats = jnp.zeros((8, DV), F32)
    for at, part in zip((0, 32, 64, 96, 112), pieces(peak, 3) + pieces(l, 2)):
        for g in range(4):
            stats = jnp.where(lane == at + g, part[8 * g : 8 * g + 8].astype(F32), stats)
    stats = stats.astype(BF16)
    for j in range(out_ref.shape[0]):
        out_ref[j, :rows, :] = o
        out_ref[j, rows:, :] = stats


def out_products(got_ref, lambda_ref, gain_ref, w_ref, out_ref):
    count = got_ref.shape[0]
    rows = 2 * SEQS
    stats = [got_ref[j, rows:, :].astype(F32) for j in range(count)]
    peaks = [x + pltpu.roll(x, 96, 1) + pltpu.roll(x, 64, 1) for x in stats]
    sums = [pltpu.roll(x, 32, 1) + pltpu.roll(x, 16, 1) for x in stats]
    peak = functools.reduce(jnp.maximum, peaks)
    scales = [jnp.exp(p - peak) for p in peaks]
    inverse = 1.0 / sum(w * l for w, l in zip(scales, sums))
    mixed = []
    for g in range(4):
        part = sum(
            w[:, g : g + 1] * got_ref[j, 8 * g : 8 * g + 8, :].astype(F32)
            for j, w in enumerate(scales)
        )
        mixed.append(part * inverse[:, g : g + 1])
    head = jnp.concatenate(mixed[:2], axis=0) - lambda_ref[:1] * jnp.concatenate(mixed[2:], axis=0)
    norm_scale = lax.rsqrt(jnp.mean(head * head, axis=1, keepdims=True) + EPSILON)
    normed = (head * norm_scale * gain_ref[...].astype(F32) * OUTPUT_KEEP).astype(BF16)
    put_copies(out_ref, 0, dot(normed, w_ref[...]).astype(BF16))


def last_sum(stream_ref, got_ref, out_ref):
    out_ref[...] = (stream_ref[...].astype(F32) + 0.5 * total(got_ref)).astype(BF16)


def local(
    tokens, lengths, cache_keys, cache_values, lambdas, head_gain, attn_gain, w_query, w_key,
    w_value, w_out, first_gain, first_gate, first_up, first_down, second_gain, second_gate,
    second_up, second_down,
):
    keys = cache_keys.reshape(SEQS, -1, 2 * DK)
    values = cache_values.reshape(SEQS, -1, DV)
    row = lambda g: g.reshape(1, -1)
    shape = jax.ShapeDtypeStruct
    wide = shape((16, SEQS, 768), BF16)
    narrow = shape((16, SEQS, 128), BF16)
    stream = shape((SEQS, 128), BF16)

    sent, lam = pl.pallas_call(
        first_products,
        out_shape=(wide, shape((8, 128), F32)),
        in_specs=[pl.BlockSpec(memory_space=pltpu.HBM)] * 5,
        out_specs=[pl.BlockSpec(memory_space=pltpu.VMEM)] * 2,
        scratch_shapes=[
            pltpu.VMEM((SEQS, 128), BF16), pltpu.VMEM((1, 128), BF16),
            pltpu.VMEM((352, 128), BF16), pltpu.VMEM((352, 128), BF16),
            pltpu.SMEM((1,), F32), pltpu.SemaphoreType.DMA((5,)),
        ],
        compiler_params=pltpu.CompilerParams(vmem_limit_bytes=60 << 20),
        cost_estimate=cost(10),
    )(tokens, row(first_gain), first_gate.T, first_up.T, lambdas)
    sent = local_call(down_products, narrow, exchange(sent, KV), first_down)
    sent, first = local_call(
        head_products, (shape((16, SEQS + 8, 128), BF16), stream),
        tokens, exchange(sent, "tp"), row(attn_gain), w_query, w_key, w_value,
    )
    sent = local_call(
        attention, shape((16, 2 * SEQS + 8, 128), BF16),
        lengths, exchange(sent, KV), keys, values, smem=(0,),
    )
    sent = local_call(
        out_products, narrow, exchange(sent, KV), lam, row(head_gain), w_out
    )
    sent, second = local_call(
        second_products, (wide, stream),
        first, exchange(sent, "tp"), row(second_gain), second_gate.T, second_up.T,
    )
    sent = local_call(down_products, narrow, exchange(sent, KV), second_down)
    return local_call(last_sum, stream, second, exchange(sent, "tp"))


def solution(mesh):
    finer = Mesh(mesh.devices.reshape(4, 4, mesh.shape["tp"]), ("kv_0", "kv_1", "tp"))
    cache = P(None, KV, "tp", None)
    placed = (
        P(None, KV), P(), cache, cache, P("tp"), P(), P(KV), P(KV, "tp"), P(KV, "tp"),
        P(KV, "tp"), P("tp", KV), P(KV), P(KV, "tp"), P(KV, "tp"), P("tp", KV), P(KV),
        P(KV, "tp"), P(KV, "tp"), P("tp", KV),
    )
    return jax.shard_map(local, mesh=finer, in_specs=placed, out_specs=P(None, KV), check_vma=False)
```

```python
import functools
import math

import jax
import jax.numpy as jnp
from jax import lax
from jax.experimental import pallas as pl
from jax.experimental.pallas import tpu as pltpu
from jax.sharding import Mesh
from jax.sharding import PartitionSpec as P

D = 2048
DK = 64
DV = 128
SEQS = 16
KV = ("kv_0", "kv_1")
EPSILON = 1e-06
ROTARY_BASE = 10000.0
OUTPUT_KEEP = 0.8
MASKED_SCORE = -1e30
F32 = jnp.float32
BF16 = jnp.bfloat16


def exchange(copies, axis):
    return lax.all_to_all(copies, axis, split_axis=0, concat_axis=0, tiled=True)


def cost(micros):
    return pl.CostEstimate(flops=int(micros * 5e8), bytes_accessed=1 << 16, transcendentals=0)


def local_call(body, outs, *arrays, scalars=0, micros=10):
    return pl.pallas_call(
        body,
        out_shape=outs,
        in_specs=[
            pl.BlockSpec(memory_space=pltpu.SMEM if i < scalars else pltpu.VMEM)
            for i in range(len(arrays))
        ],
        out_specs=jax.tree.map(lambda _: pl.BlockSpec(memory_space=pltpu.VMEM), outs),
        compiler_params=pltpu.CompilerParams(vmem_limit_bytes=4 << 20),
        cost_estimate=cost(micros),
    )(*arrays)


def dot_rows(a, b):
    return lax.dot_general(a, b, (((1,), (1,)), ((), ())), preferred_element_type=F32)


def dot(a, b):
    return jnp.dot(a, b, preferred_element_type=F32)


def put_copies(out_ref, at, value):
    for j in range(out_ref.shape[0]):
        out_ref[j, :, at : at + value.shape[1]] = value


def pieces(value, count):
    parts = []
    for _ in range(count):
        part = value.astype(BF16)
        parts.append(part)
        value = value - part.astype(F32)
    return parts


def with_columns(width, columns):
    lane = lax.broadcasted_iota(jnp.int32, (columns[0].shape[0], width), 1)
    out = jnp.zeros(lane.shape, F32)
    for i, c in enumerate(columns):
        out = jnp.where(lane == i, c.astype(F32), out)
    return out.astype(BF16)


def total(ref):
    out = ref[0].astype(F32)
    for j in range(1, ref.shape[0]):
        out = out + ref[j].astype(F32)
    return out


def gate_up_products(stream_f, gain_ref, gate_ref, up_ref, out_ref):
    scaled = (stream_f * gain_ref[...].astype(F32)).astype(BF16)
    square = jnp.sum(stream_f * stream_f, axis=1, keepdims=True)
    gate = dot_rows(scaled, gate_ref[...]).astype(BF16)
    up = dot_rows(scaled, up_ref[...]).astype(BF16)
    put_copies(out_ref, 0, gate)
    put_copies(out_ref, 352, with_columns(32, pieces(square, 2)))
    put_copies(out_ref, 384, up)
    put_copies(out_ref, 736, jnp.zeros((SEQS, 32), BF16))


def rotary_steps(steps_ref):
    half = DK // 2
    lane = lax.broadcasted_iota(jnp.int32, steps_ref.shape, 1)
    steps_ref[...] = jnp.exp((lane % half).astype(F32) * (-math.log(ROTARY_BASE) / half))


def side_tables(lengths_ref, lambda_ref, steps_ref, side_ref, limit_ref):
    row = lax.broadcasted_iota(jnp.int32, steps_ref.shape, 0)
    limit = jnp.zeros(steps_ref.shape, jnp.int32)
    for b in range(SEQS):
        limit = jnp.where(row == b, lengths_ref[b], limit)
    for part in range(4):
        limit_ref[8 * part : 8 * part + 8, :] = limit[8 * (part // 2) : 8 * (part // 2) + 8]
    angles = limit.astype(F32) * steps_ref[...]
    lane = lax.broadcasted_iota(jnp.int32, angles.shape, 1)
    sine = jnp.sin(angles)
    side_ref[0] = jnp.cos(angles)
    side_ref[1] = jnp.where((lane & (DK // 2)) == 0, -sine, sine)
    side_ref[2] = jnp.full(angles.shape, lambda_ref[0], F32)


def first_products(tokens_ref, gain_ref, gate_ref, up_ref, side_ref, out_ref):
    gate_up_products(tokens_ref[...].astype(F32), gain_ref, gate_ref, up_ref, out_ref)


def second_products(stream_ref, got_ref, gain_ref, gate_ref, up_ref, out_ref, second_ref):
    second = (stream_ref[...].astype(F32) + total(got_ref)).astype(BF16)
    second_ref[...] = second
    gate_up_products(second.astype(F32), gain_ref, gate_ref, up_ref, out_ref)


def down_products(got_ref, down_ref, out_ref):
    summed = total(got_ref)
    square = summed[:, 352:353] + summed[:, 353:354]
    row_scale = lax.rsqrt(square / D + EPSILON)
    gate = row_scale * summed[:, :352]
    up = row_scale * summed[:, 384:736]
    hidden = (gate / (1.0 + jnp.exp(-gate)) * up).astype(BF16)
    put_copies(out_ref, 0, dot(hidden, down_ref[...]).astype(BF16))


def head_products(tokens_ref, got_ref, gain_ref, wq_ref, wk_ref, wv_ref, out_ref, first_ref):
    first = (tokens_ref[...].astype(F32) + 0.5 * total(got_ref)).astype(BF16)
    first_ref[...] = first
    stream_f = first.astype(F32)
    scaled = (stream_f * gain_ref[...].astype(F32)).astype(BF16)
    square = jnp.sum(stream_f * stream_f, axis=1, keepdims=True)
    query = dot(scaled, wq_ref[...]).astype(BF16)
    key = dot(scaled, wk_ref[...])
    value = dot(scaled, wv_ref[...])
    diagonal = lax.broadcasted_iota(jnp.int32, (SEQS, 128), 0) == lax.broadcasted_iota(
        jnp.int32, (SEQS, 128), 1
    )
    high, rest = pieces(jnp.sum(jnp.where(diagonal, square, 0.0), axis=0, keepdims=True), 2)
    row = lax.broadcasted_iota(jnp.int32, (8, 128), 0)
    squares = jnp.where(row == 2, high.astype(F32), jnp.where(row == 3, rest.astype(F32), 0.0))
    for j in range(SEQS):
        out_ref[j, :SEQS, :] = query
        tail = jnp.where(row == 0, key[j : j + 1], jnp.where(row == 1, value[j : j + 1], squares))
        out_ref[j, SEQS:, :] = tail.astype(BF16)


def attention(got_ref, side_ref, limit_ref, keys_ref, values_ref, out_ref):
    summed = total(got_ref)
    cosine, sine = side_ref[0], side_ref[1]
    lane = lax.broadcasted_iota(jnp.int32, cosine.shape, 1)
    row = lax.broadcasted_iota(jnp.int32, cosine.shape, 0)
    low = (lane & (DK // 2)) == 0
    kv_index = lax.axis_index(KV)
    mine = row == kv_index
    square = jnp.sum(
        jnp.where(row == lane, summed[18:19] + summed[19:20], 0.0), axis=1, keepdims=True
    )
    row_scale = lax.rsqrt(square / D + EPSILON)

    def of_mine(x):
        return jnp.sum(jnp.where(mine, x, 0.0), axis=0, keepdims=True)

    def rotate(x, cosine, sine, low):
        swapped = jnp.where(low, pltpu.roll(x, 96, 1), pltpu.roll(x, 32, 1))
        return (x * cosine + swapped * sine).astype(BF16).astype(F32)

    def eight(x):
        return jnp.broadcast_to(x, (8, x.shape[1]))

    query = rotate(row_scale * summed[:SEQS], cosine, sine, low)
    my_scale = of_mine(jnp.broadcast_to(row_scale, lane.shape))
    key_new = rotate(
        eight(my_scale * summed[16:17]), eight(of_mine(cosine)), eight(of_mine(sine)), low[:8]
    )[:1]
    value_new = (my_scale * summed[17:18]).astype(BF16).astype(F32)
    scale_att = DK ** (-0.5)
    first_part = lane < DK
    parts = jnp.where(first_part, query, 0.0), jnp.where(first_part, 0.0, query)
    both = jnp.concatenate([p[8 * g : 8 * g + 8] for g in range(2) for p in parts], axis=0)
    rows = 2 * SEQS
    positions = keys_ref.shape[1]
    of_row = lax.broadcasted_iota(jnp.int32, (SEQS, DV), 0) % 8
    place = lax.broadcasted_iota(jnp.int32, (SEQS, positions), 1) + kv_index * positions
    scores = []
    for g in range(2):
        s = jnp.zeros((SEQS, positions), F32)
        for b in range(8):
            picked = jnp.where(of_row == b, both[SEQS * g : SEQS * g + SEQS], 0.0).astype(BF16)
            s = s + dot_rows(picked, keys_ref[8 * g + b])
        scores.append(s)
    found = []
    for g, s in enumerate(scores):
        alive = place < limit_ref[SEQS * g : SEQS * g + SEQS, :1]
        s = jnp.where(alive, s * scale_att, MASKED_SCORE)
        top = jnp.max(s, axis=1, keepdims=True)
        e = jnp.where(alive, jnp.exp(s - top), 0.0)
        weights = e.astype(BF16)
        o = jnp.zeros((SEQS, DV), F32)
        for b in range(8):
            o = jnp.where(of_row == b, dot(weights, values_ref[8 * g + b]), o)
        found.append((top, jnp.sum(e, axis=1, keepdims=True), o))
    old, l, o = (jnp.concatenate(pair, axis=0) for pair in zip(*found))
    line = lax.broadcasted_iota(jnp.int32, (rows, 1), 0)
    here = line // SEQS * 8 + line % 8 == kv_index
    own_score = scale_att * jnp.sum(both * key_new, axis=1, keepdims=True)
    own_score = jnp.where(here, own_score, MASKED_SCORE)
    peak = jnp.maximum(old, own_score)
    old_scale = jnp.exp(old - peak)
    fresh = jnp.where(here, jnp.exp(own_score - peak), 0.0)
    l = l * old_scale + fresh
    o = (o * old_scale + fresh * value_new).astype(BF16)
    lane = lane[:8]
    stats = jnp.zeros((8, DV), F32)
    for at, part in zip((0, 32, 64, 96, 112), pieces(peak, 3) + pieces(l, 2)):
        for g in range(4):
            stats = jnp.where(lane == at + g, part[8 * g : 8 * g + 8].astype(F32), stats)
    stats = stats.astype(BF16)
    for j in range(out_ref.shape[0]):
        out_ref[j, :rows, :] = o
        out_ref[j, rows:, :] = stats


def out_products(got_ref, side_ref, gain_ref, w_ref, out_ref):
    count = got_ref.shape[0]
    rows = 2 * SEQS
    stats = [got_ref[j, rows:, :].astype(F32) for j in range(count)]
    peaks = [x + pltpu.roll(x, 96, 1) + pltpu.roll(x, 64, 1) for x in stats]
    sums = [pltpu.roll(x, 32, 1) + pltpu.roll(x, 16, 1) for x in stats]
    peak = functools.reduce(jnp.maximum, peaks)
    scales = [jnp.exp(p - peak) for p in peaks]
    inverse = 1.0 / sum(w * l for w, l in zip(scales, sums))
    mixed = []
    for g in range(4):
        part = sum(
            w[:, g : g + 1] * got_ref[j, 8 * g : 8 * g + 8, :].astype(F32)
            for j, w in enumerate(scales)
        )
        mixed.append(part * inverse[:, g : g + 1])
    head = jnp.concatenate(mixed[::2], axis=0) - side_ref[2] * jnp.concatenate(mixed[1::2], axis=0)
    norm_scale = lax.rsqrt(jnp.mean(head * head, axis=1, keepdims=True) + EPSILON)
    normed = (head * norm_scale * gain_ref[...].astype(F32) * OUTPUT_KEEP).astype(BF16)
    put_copies(out_ref, 0, dot(normed, w_ref[...]).astype(BF16))


def last_sum(stream_ref, got_ref, out_ref):
    out_ref[...] = (stream_ref[...].astype(F32) + 0.5 * total(got_ref)).astype(BF16)


def local(
    tokens, lengths, cache_keys, cache_values, lambdas, head_gain, attn_gain, w_query, w_key,
    w_value, w_out, first_gain, first_gate, first_up, first_down, second_gain, second_gate,
    second_up, second_down,
):
    keys = cache_keys.reshape(SEQS, -1, 2 * DK)
    values = cache_values.reshape(SEQS, -1, DV)
    row = lambda g: g.reshape(1, -1)
    shape = jax.ShapeDtypeStruct
    wide = shape((16, SEQS, 768), BF16)
    narrow = shape((16, SEQS, 128), BF16)
    stream = shape((SEQS, 128), BF16)

    steps = local_call(rotary_steps, shape((SEQS, 128), F32))
    side, limit = local_call(
        side_tables, (shape((3, SEQS, 128), F32), shape((2 * SEQS, 128), jnp.int32)),
        lengths, lambdas, steps, scalars=2, micros=0.01,
    )
    sent = local_call(
        first_products, wide, tokens, row(first_gain), first_gate.T, first_up.T, side
    )
    sent = local_call(down_products, narrow, exchange(sent, KV), first_down)
    sent, first = local_call(
        head_products, (shape((16, SEQS + 8, 128), BF16), stream),
        tokens, exchange(sent, "tp"), row(attn_gain), w_query, w_key, w_value,
    )
    sent = local_call(
        attention, shape((16, 2 * SEQS + 8, 128), BF16),
        exchange(sent, KV), side, limit, keys, values,
    )
    sent = local_call(
        out_products, narrow, exchange(sent, KV), side, row(head_gain), w_out
    )
    sent, second = local_call(
        second_products, (wide, stream),
        first, exchange(sent, "tp"), row(second_gain), second_gate.T, second_up.T,
    )
    sent = local_call(down_products, narrow, exchange(sent, KV), second_down)
    return local_call(last_sum, stream, second, exchange(sent, "tp"))


def solution(mesh):
    finer = Mesh(mesh.devices.reshape(4, 4, mesh.shape["tp"]), ("kv_0", "kv_1", "tp"))
    cache = P(None, KV, "tp", None)
    placed = (
        P(None, KV), P(), cache, cache, P("tp"), P(), P(KV), P(KV, "tp"), P(KV, "tp"),
        P(KV, "tp"), P("tp", KV), P(KV), P(KV, "tp"), P(KV, "tp"), P("tp", KV), P(KV),
        P(KV, "tp"), P(KV, "tp"), P("tp", KV),
    )
    return jax.shard_map(local, mesh=finer, in_specs=placed, out_specs=P(None, KV), check_vma=False)
```

```python
import functools
import math

import jax
import jax.numpy as jnp
from jax import lax
from jax.experimental import pallas as pl
from jax.experimental.pallas import tpu as pltpu
from jax.sharding import Mesh
from jax.sharding import PartitionSpec as P

D = 2048
DK = 64
DV = 128
SEQS = 16
KV = ("kv_0", "kv_1")
EPSILON = 1e-06
ROTARY_BASE = 10000.0
OUTPUT_KEEP = 0.8
MASKED_SCORE = -1e30
F32 = jnp.float32
BF16 = jnp.bfloat16


def exchange(copies, axis):
    return lax.all_to_all(copies, axis, split_axis=0, concat_axis=0, tiled=True)


def cost(micros):
    return pl.CostEstimate(flops=int(micros * 5e8), bytes_accessed=1 << 16, transcendentals=0)


def local_call(body, outs, *arrays, scalars=0, micros=10):
    return pl.pallas_call(
        body,
        out_shape=outs,
        in_specs=[
            pl.BlockSpec(memory_space=pltpu.SMEM if i < scalars else pltpu.VMEM)
            for i in range(len(arrays))
        ],
        out_specs=jax.tree.map(lambda _: pl.BlockSpec(memory_space=pltpu.VMEM), outs),
        compiler_params=pltpu.CompilerParams(vmem_limit_bytes=4 << 20),
        cost_estimate=cost(micros),
    )(*arrays)


def dot_rows(a, b):
    return lax.dot_general(a, b, (((1,), (1,)), ((), ())), preferred_element_type=F32)


def dot(a, b):
    return jnp.dot(a, b, preferred_element_type=F32)


def put_copies(out_ref, at, value):
    for j in range(out_ref.shape[0]):
        out_ref[j, :, at : at + value.shape[1]] = value


def pieces(value, count):
    parts = []
    for _ in range(count):
        part = value.astype(BF16)
        parts.append(part)
        value = value - part.astype(F32)
    return parts


def with_columns(width, columns):
    lane = lax.broadcasted_iota(jnp.int32, (columns[0].shape[0], width), 1)
    out = jnp.zeros(lane.shape, F32)
    for i, c in enumerate(columns):
        out = jnp.where(lane == i, c.astype(F32), out)
    return out.astype(BF16)


def total(ref):
    out = ref[0].astype(F32)
    for j in range(1, ref.shape[0]):
        out = out + ref[j].astype(F32)
    return out


def gate_up_products(stream_f, gain_ref, gate_ref, up_ref, out_ref):
    scaled = (stream_f * gain_ref[...].astype(F32)).astype(BF16)
    square = jnp.sum(stream_f * stream_f, axis=1, keepdims=True)
    gate = dot_rows(scaled, gate_ref[...]).astype(BF16)
    up = dot_rows(scaled, up_ref[...]).astype(BF16)
    put_copies(out_ref, 0, gate)
    put_copies(out_ref, 352, with_columns(32, pieces(square, 2)))
    put_copies(out_ref, 384, up)
    put_copies(out_ref, 736, jnp.zeros((SEQS, 32), BF16))


def rotary_steps(steps_ref):
    half = DK // 2
    lane = lax.broadcasted_iota(jnp.int32, steps_ref.shape, 1)
    steps_ref[...] = jnp.exp((lane % half).astype(F32) * (-math.log(ROTARY_BASE) / half))


def side_tables(lambda_ref, lengths_ref, steps_ref, side_ref, limit_ref):
    lane = lax.broadcasted_iota(jnp.int32, (SEQS, SEQS), 1)
    row = lax.broadcasted_iota(jnp.int32, (SEQS, SEQS), 0)
    limit = jnp.sum(
        jnp.where(lane == row, lengths_ref[...].astype(F32), 0.0), axis=1, keepdims=True
    )
    for part in range(4):
        limit_ref[8 * part : 8 * part + 8, :] = jnp.broadcast_to(
            limit[8 * (part // 2) : 8 * (part // 2) + 8].astype(jnp.int32), (8, 128)
        )
    angles = limit * steps_ref[...]
    sine = jnp.sin(angles)
    lane = lax.broadcasted_iota(jnp.int32, angles.shape, 1)
    side_ref[0] = jnp.cos(angles)
    side_ref[1] = jnp.where((lane & (DK // 2)) == 0, -sine, sine)
    side_ref[2] = jnp.full(angles.shape, lambda_ref[0], F32)


def first_products(tokens_ref, gain_ref, gate_ref, up_ref, side_ref, out_ref):
    gate_up_products(tokens_ref[...].astype(F32), gain_ref, gate_ref, up_ref, out_ref)


def second_products(stream_ref, got_ref, gain_ref, gate_ref, up_ref, out_ref, second_ref):
    second = (stream_ref[...].astype(F32) + total(got_ref)).astype(BF16)
    second_ref[...] = second
    gate_up_products(second.astype(F32), gain_ref, gate_ref, up_ref, out_ref)


def down_products(got_ref, down_ref, out_ref):
    summed = total(got_ref)
    square = summed[:, 352:353] + summed[:, 353:354]
    row_scale = lax.rsqrt(square / D + EPSILON)
    gate = row_scale * summed[:, :352]
    up = row_scale * summed[:, 384:736]
    hidden = (gate / (1.0 + jnp.exp(-gate)) * up).astype(BF16)
    put_copies(out_ref, 0, dot(hidden, down_ref[...]).astype(BF16))


def head_products(tokens_ref, got_ref, gain_ref, wq_ref, wk_ref, wv_ref, out_ref, first_ref):
    first = (tokens_ref[...].astype(F32) + 0.5 * total(got_ref)).astype(BF16)
    first_ref[...] = first
    stream_f = first.astype(F32)
    scaled = (stream_f * gain_ref[...].astype(F32)).astype(BF16)
    square = jnp.sum(stream_f * stream_f, axis=1, keepdims=True)
    query = dot(scaled, wq_ref[...]).astype(BF16)
    key = dot(scaled, wk_ref[...])
    value = dot(scaled, wv_ref[...])
    diagonal = lax.broadcasted_iota(jnp.int32, (SEQS, 128), 0) == lax.broadcasted_iota(
        jnp.int32, (SEQS, 128), 1
    )
    high, rest = pieces(jnp.sum(jnp.where(diagonal, square, 0.0), axis=0, keepdims=True), 2)
    row = lax.broadcasted_iota(jnp.int32, (8, 128), 0)
    squares = jnp.where(row == 2, high.astype(F32), jnp.where(row == 3, rest.astype(F32), 0.0))
    for j in range(SEQS):
        out_ref[j, :SEQS, :] = query
        tail = jnp.where(row == 0, key[j : j + 1], jnp.where(row == 1, value[j : j + 1], squares))
        out_ref[j, SEQS:, :] = tail.astype(BF16)


def attention(got_ref, side_ref, limit_ref, keys_ref, values_ref, out_ref):
    summed = total(got_ref)
    cosine, sine = side_ref[0], side_ref[1]
    lane = lax.broadcasted_iota(jnp.int32, cosine.shape, 1)
    row = lax.broadcasted_iota(jnp.int32, cosine.shape, 0)
    low = (lane & (DK // 2)) == 0
    kv_index = lax.axis_index(KV)
    mine = row == kv_index
    square = jnp.sum(
        jnp.where(row == lane, summed[18:19] + summed[19:20], 0.0), axis=1, keepdims=True
    )
    row_scale = lax.rsqrt(square / D + EPSILON)

    def of_mine(x):
        return jnp.sum(jnp.where(mine, x, 0.0), axis=0, keepdims=True)

    def rotate(x, cosine, sine, low):
        swapped = jnp.where(low, pltpu.roll(x, 96, 1), pltpu.roll(x, 32, 1))
        return (x * cosine + swapped * sine).astype(BF16).astype(F32)

    def eight(x):
        return jnp.broadcast_to(x, (8, x.shape[1]))

    query = rotate(row_scale * summed[:SEQS], cosine, sine, low)
    my_scale = of_mine(jnp.broadcast_to(row_scale, lane.shape))
    key_new = rotate(
        eight(my_scale * summed[16:17]), eight(of_mine(cosine)), eight(of_mine(sine)), low[:8]
    )[:1]
    value_new = (my_scale * summed[17:18]).astype(BF16).astype(F32)
    scale_att = DK ** (-0.5)
    first_part = lane < DK
    parts = jnp.where(first_part, query, 0.0), jnp.where(first_part, 0.0, query)
    both = jnp.concatenate([p[8 * g : 8 * g + 8] for g in range(2) for p in parts], axis=0)
    rows = 2 * SEQS
    positions = keys_ref.shape[1]
    of_row = lax.broadcasted_iota(jnp.int32, (SEQS, DV), 0) % 8
    place = lax.broadcasted_iota(jnp.int32, (SEQS, positions), 1) + kv_index * positions
    scores = []
    for g in range(2):
        s = jnp.zeros((SEQS, positions), F32)
        for b in range(8):
            picked = jnp.where(of_row == b, both[SEQS * g : SEQS * g + SEQS], 0.0).astype(BF16)
            s = s + dot_rows(picked, keys_ref[8 * g + b])
        scores.append(s)
    found = []
    for g, s in enumerate(scores):
        alive = place < limit_ref[SEQS * g : SEQS * g + SEQS, :1]
        s = jnp.where(alive, s * scale_att, MASKED_SCORE)
        top = jnp.max(s, axis=1, keepdims=True)
        e = jnp.where(alive, jnp.exp(s - top), 0.0)
        weights = e.astype(BF16)
        o = jnp.zeros((SEQS, DV), F32)
        for b in range(8):
            o = jnp.where(of_row == b, dot(weights, values_ref[8 * g + b]), o)
        found.append((top, jnp.sum(e, axis=1, keepdims=True), o))
    old, l, o = (jnp.concatenate(pair, axis=0) for pair in zip(*found))
    line = lax.broadcasted_iota(jnp.int32, (rows, 1), 0)
    here = line // SEQS * 8 + line % 8 == kv_index
    own_score = scale_att * jnp.sum(both * key_new, axis=1, keepdims=True)
    own_score = jnp.where(here, own_score, MASKED_SCORE)
    peak = jnp.maximum(old, own_score)
    old_scale = jnp.exp(old - peak)
    fresh = jnp.where(here, jnp.exp(own_score - peak), 0.0)
    l = l * old_scale + fresh
    o = (o * old_scale + fresh * value_new).astype(BF16)
    lane = lane[:8]
    stats = jnp.zeros((8, DV), F32)
    for at, part in zip((0, 32, 64, 96, 112), pieces(peak, 3) + pieces(l, 2)):
        for g in range(4):
            stats = jnp.where(lane == at + g, part[8 * g : 8 * g + 8].astype(F32), stats)
    stats = stats.astype(BF16)
    for j in range(out_ref.shape[0]):
        out_ref[j, :rows, :] = o
        out_ref[j, rows:, :] = stats


def out_products(got_ref, side_ref, gain_ref, w_ref, out_ref):
    count = got_ref.shape[0]
    rows = 2 * SEQS
    stats = [got_ref[j, rows:, :].astype(F32) for j in range(count)]
    peaks = [x + pltpu.roll(x, 96, 1) + pltpu.roll(x, 64, 1) for x in stats]
    sums = [pltpu.roll(x, 32, 1) + pltpu.roll(x, 16, 1) for x in stats]
    peak = functools.reduce(jnp.maximum, peaks)
    scales = [jnp.exp(p - peak) for p in peaks]
    inverse = 1.0 / sum(w * l for w, l in zip(scales, sums))
    mixed = []
    for g in range(4):
        part = sum(
            w[:, g : g + 1] * got_ref[j, 8 * g : 8 * g + 8, :].astype(F32)
            for j, w in enumerate(scales)
        )
        mixed.append(part * inverse[:, g : g + 1])
    head = jnp.concatenate(mixed[::2], axis=0) - side_ref[2] * jnp.concatenate(mixed[1::2], axis=0)
    norm_scale = lax.rsqrt(jnp.mean(head * head, axis=1, keepdims=True) + EPSILON)
    normed = (head * norm_scale * gain_ref[...].astype(F32) * OUTPUT_KEEP).astype(BF16)
    put_copies(out_ref, 0, dot(normed, w_ref[...]).astype(BF16))


def last_sum(stream_ref, got_ref, out_ref):
    out_ref[...] = (stream_ref[...].astype(F32) + 0.5 * total(got_ref)).astype(BF16)


def local(
    tokens, lengths, cache_keys, cache_values, lambdas, head_gain, attn_gain, w_query, w_key,
    w_value, w_out, first_gain, first_gate, first_up, first_down, second_gain, second_gate,
    second_up, second_down,
):
    keys = cache_keys.reshape(SEQS, -1, 2 * DK)
    values = cache_values.reshape(SEQS, -1, DV)
    row = lambda g: g.reshape(1, -1)
    shape = jax.ShapeDtypeStruct
    wide = shape((16, SEQS, 768), BF16)
    narrow = shape((16, SEQS, 128), BF16)
    stream = shape((SEQS, 128), BF16)

    steps = local_call(rotary_steps, shape((SEQS, 128), F32))
    side, limit = local_call(
        side_tables, (shape((3, SEQS, 128), F32), shape((2 * SEQS, 128), jnp.int32)),
        lambdas, row(lengths), steps, scalars=1, micros=0.01,
    )
    sent = local_call(
        first_products, wide, tokens, row(first_gain), first_gate.T, first_up.T, side
    )
    sent = local_call(down_products, narrow, exchange(sent, KV), first_down)
    sent, first = local_call(
        head_products, (shape((16, SEQS + 8, 128), BF16), stream),
        tokens, exchange(sent, "tp"), row(attn_gain), w_query, w_key, w_value,
    )
    sent = local_call(
        attention, shape((16, 2 * SEQS + 8, 128), BF16),
        exchange(sent, KV), side, limit, keys, values,
    )
    sent = local_call(
        out_products, narrow, exchange(sent, KV), side, row(head_gain), w_out
    )
    sent, second = local_call(
        second_products, (wide, stream),
        first, exchange(sent, "tp"), row(second_gain), second_gate.T, second_up.T,
    )
    sent = local_call(down_products, narrow, exchange(sent, KV), second_down)
    return local_call(last_sum, stream, second, exchange(sent, "tp"))


def solution(mesh):
    finer = Mesh(mesh.devices.reshape(4, 4, mesh.shape["tp"]), ("kv_0", "kv_1", "tp"))
    cache = P(None, KV, "tp", None)
    placed = (
        P(None, KV), P(), cache, cache, P("tp"), P(), P(KV), P(KV, "tp"), P(KV, "tp"),
        P(KV, "tp"), P("tp", KV), P(KV), P(KV, "tp"), P(KV, "tp"), P("tp", KV), P(KV),
        P(KV, "tp"), P(KV, "tp"), P("tp", KV),
    )
    return jax.shard_map(local, mesh=finer, in_specs=placed, out_specs=P(None, KV), check_vma=False)
```

```python
import functools
import math

import jax
import jax.numpy as jnp
from jax import lax
from jax.experimental import pallas as pl
from jax.experimental.pallas import tpu as pltpu
from jax.sharding import Mesh
from jax.sharding import PartitionSpec as P

D = 2048
DK = 64
DV = 128
SEQS = 16
KV = ("kv_0", "kv_a", "kv_b")
HALF = ("kv_0", "kv_b")
PAIR = [(x, 3 - x) for x in range(4)]
EPSILON = 1e-06
ROTARY_BASE = 10000.0
OUTPUT_KEEP = 0.8
MASKED_SCORE = -1e30
GATE, UP, W_OUT, TOKENS, GAINS, PACK = 384, 736, 1088, 1216, 1232, 1264
F32 = jnp.float32
BF16 = jnp.bfloat16


def exchange(copies, axis):
    return lax.all_to_all(copies, axis, split_axis=0, concat_axis=0, tiled=True)


def cost(micros):
    return pl.CostEstimate(flops=int(micros * 5e8), bytes_accessed=1 << 16, transcendentals=0)


def local_call(body, outs, *arrays, scalars=0, micros=10):
    return pl.pallas_call(
        body,
        out_shape=outs,
        in_specs=[
            pl.BlockSpec(memory_space=pltpu.SMEM if i < scalars else pltpu.VMEM)
            for i in range(len(arrays))
        ],
        out_specs=jax.tree.map(lambda _: pl.BlockSpec(memory_space=pltpu.VMEM), outs),
        compiler_params=pltpu.CompilerParams(vmem_limit_bytes=4 << 20),
        cost_estimate=cost(micros),
    )(*arrays)


def dot_rows(a, b):
    return lax.dot_general(a, b, (((1,), (1,)), ((), ())), preferred_element_type=F32)


def dot(a, b):
    return jnp.dot(a, b, preferred_element_type=F32)


def put_copies(out_ref, at, value):
    for j in range(out_ref.shape[0]):
        out_ref[j, :, at : at + value.shape[1]] = value


def pieces(value, count):
    parts = []
    for _ in range(count):
        part = value.astype(BF16)
        parts.append(part)
        value = value - part.astype(F32)
    return parts


def with_columns(width, columns):
    lane = lax.broadcasted_iota(jnp.int32, (columns[0].shape[0], width), 1)
    out = jnp.zeros(lane.shape, F32)
    for i, c in enumerate(columns):
        out = jnp.where(lane == i, c.astype(F32), out)
    return out.astype(BF16)


def total(ref):
    out = ref[0].astype(F32)
    for j in range(1, ref.shape[0]):
        out = out + ref[j].astype(F32)
    return out


def gate_up_products(streams, gains, gates, ups, out_ref):
    scaled = [(x * g.astype(F32)).astype(BF16) for x, g in zip(streams, gains)]
    square = sum(jnp.sum(x * x, axis=1, keepdims=True) for x in streams)
    put_copies(out_ref, 0, sum(map(dot_rows, scaled, gates)).astype(BF16))
    put_copies(out_ref, 352, with_columns(32, pieces(square, 2)))
    put_copies(out_ref, 384, sum(map(dot_rows, scaled, ups)).astype(BF16))
    put_copies(out_ref, 736, jnp.zeros((SEQS, 32), BF16))


def rotary_steps(steps_ref):
    half = DK // 2
    lane = lax.broadcasted_iota(jnp.int32, steps_ref.shape, 1)
    steps_ref[...] = jnp.exp((lane % half).astype(F32) * (-math.log(ROTARY_BASE) / half))


def side_tables(lambda_ref, lengths_ref, steps_ref, side_ref, limit_ref):
    lane = lax.broadcasted_iota(jnp.int32, (SEQS, SEQS), 1)
    row = lax.broadcasted_iota(jnp.int32, (SEQS, SEQS), 0)
    limit = jnp.sum(
        jnp.where(lane == row, lengths_ref[...].astype(F32), 0.0), axis=1, keepdims=True
    )
    for part in range(4):
        limit_ref[8 * part : 8 * part + 8, :] = jnp.broadcast_to(
            limit[8 * (part // 2) : 8 * (part // 2) + 8].astype(jnp.int32), (8, 128)
        )
    angles = limit * steps_ref[...]
    sine = jnp.sin(angles)
    lane = lax.broadcasted_iota(jnp.int32, angles.shape, 1)
    side_ref[0] = jnp.cos(angles)
    side_ref[1] = jnp.where((lane & (DK // 2)) == 0, -sine, sine)
    side_ref[2] = jnp.full(angles.shape, lambda_ref[0], F32)


def first_products(tokens_ref, gain_ref, gate_ref, up_ref, side_ref, out_ref):
    gate_up_products(
        [tokens_ref[...].astype(F32)], [gain_ref[...]], [gate_ref[...]], [up_ref[...]], out_ref
    )


def second_products(stream_ref, got_ref, gain_ref, gate_ref, up_ref, pack_ref, out_ref, second_ref):
    second = (stream_ref[...].astype(F32) + total(got_ref)).astype(BF16)
    second_ref[...] = second[:, :128]
    second = second.astype(F32)
    gate_up_products(
        [second[:, :128], second[:, 128:]],
        [gain_ref[...], pack_ref[GAINS + 16 : GAINS + 17]],
        [gate_ref[...], pack_ref[GATE : GATE + 352]],
        [up_ref[...], pack_ref[UP : UP + 352]],
        out_ref,
    )


def hidden_units(got_ref):
    summed = total(got_ref)
    square = summed[:, 352:353] + summed[:, 353:354]
    row_scale = lax.rsqrt(square / D + EPSILON)
    gate = row_scale * summed[:, :352]
    up = row_scale * summed[:, 384:736]
    return (gate / (1.0 + jnp.exp(-gate)) * up).astype(BF16)


def hidden_and_pack(
    got_ref, wq_ref, wk_ref, wv_ref, gate_ref, up_ref, w_out_ref, tokens_ref, attn_gain_ref,
    second_gain_ref, hidden_ref, pack_ref
):
    hidden_ref[...] = hidden_units(got_ref)
    at = 0
    for ref in (wq_ref, wk_ref, wv_ref, gate_ref, up_ref, w_out_ref, tokens_ref):
        pack_ref[at : at + ref.shape[0], :] = ref[...]
        at += ref.shape[0]
    for ref in (attn_gain_ref, second_gain_ref):
        pack_ref[at : at + 16, :] = jnp.broadcast_to(ref[...], (16, 128))
        at += 16


def down_products_of_pair(hidden_ref, down_ref, other_ref, out_ref):
    hidden = hidden_ref[...]
    put_copies(out_ref, 0, dot(hidden, down_ref[...]).astype(BF16))
    put_copies(out_ref, 128, dot(hidden, other_ref[...]).astype(BF16))


def down_products(got_ref, down_ref, out_ref):
    put_copies(out_ref, 0, dot(hidden_units(got_ref), down_ref[...]).astype(BF16))


def head_products(
    tokens_ref, got_ref, gain_ref, wq_ref, wk_ref, wv_ref, pack_ref, out_ref, first_ref
):
    tokens = jnp.concatenate([tokens_ref[...], pack_ref[TOKENS : TOKENS + 16]], axis=1)
    first = (tokens.astype(F32) + 0.5 * total(got_ref)).astype(BF16)
    first_ref[...] = first
    stream_f = first.astype(F32)
    square = jnp.sum(stream_f * stream_f, axis=1, keepdims=True)
    own = (stream_f[:, :128] * gain_ref[...].astype(F32)).astype(BF16)
    other = (stream_f[:, 128:] * pack_ref[GAINS : GAINS + 1].astype(F32)).astype(BF16)
    query, key, value = (
        dot(own, ref[...]) + dot(other, pack_ref[128 * i : 128 * i + 128])
        for i, ref in enumerate((wq_ref, wk_ref, wv_ref))
    )
    query = query.astype(BF16)
    diagonal = lax.broadcasted_iota(jnp.int32, (SEQS, 128), 0) == lax.broadcasted_iota(
        jnp.int32, (SEQS, 128), 1
    )
    high, rest = pieces(jnp.sum(jnp.where(diagonal, square, 0.0), axis=0, keepdims=True), 2)
    row = lax.broadcasted_iota(jnp.int32, (8, 128), 0)
    squares = jnp.where(row == 2, high.astype(F32), jnp.where(row == 3, rest.astype(F32), 0.0))
    near = lax.axis_index("kv_a") == 0

    def row_of(x, peer):
        at = 4 * (peer // 2) + peer % 2
        return jnp.where(near, x[at : at + 1], x[at + 2 : at + 3])

    for j in range(out_ref.shape[0]):
        out_ref[j, :SEQS, :] = query
        tail = jnp.where(row == 0, row_of(key, j), jnp.where(row == 1, row_of(value, j), squares))
        out_ref[j, SEQS:, :] = tail.astype(BF16)


def attention(got_ref, side_ref, limit_ref, keys_ref, values_ref, out_ref):
    summed = total(got_ref)
    cosine, sine = side_ref[0], side_ref[1]
    lane = lax.broadcasted_iota(jnp.int32, cosine.shape, 1)
    row = lax.broadcasted_iota(jnp.int32, cosine.shape, 0)
    low = (lane & (DK // 2)) == 0
    kv_index = lax.axis_index(KV)
    mine = row == kv_index
    square = jnp.sum(
        jnp.where(row == lane, summed[18:19] + summed[19:20], 0.0), axis=1, keepdims=True
    )
    row_scale = lax.rsqrt(square / D + EPSILON)

    def of_mine(x):
        return jnp.sum(jnp.where(mine, x, 0.0), axis=0, keepdims=True)

    def rotate(x, cosine, sine, low):
        swapped = jnp.where(low, pltpu.roll(x, 96, 1), pltpu.roll(x, 32, 1))
        return (x * cosine + swapped * sine).astype(BF16).astype(F32)

    def eight(x):
        return jnp.broadcast_to(x, (8, x.shape[1]))

    query = rotate(row_scale * summed[:SEQS], cosine, sine, low)
    my_scale = of_mine(jnp.broadcast_to(row_scale, lane.shape))
    key_new = rotate(
        eight(my_scale * summed[16:17]), eight(of_mine(cosine)), eight(of_mine(sine)), low[:8]
    )[:1]
    value_new = (my_scale * summed[17:18]).astype(BF16).astype(F32)
    scale_att = DK ** (-0.5)
    first_part = lane < DK
    parts = jnp.where(first_part, query, 0.0), jnp.where(first_part, 0.0, query)
    both = jnp.concatenate([p[8 * g : 8 * g + 8] for g in range(2) for p in parts], axis=0)
    rows = 2 * SEQS
    positions = keys_ref.shape[1]
    of_row = lax.broadcasted_iota(jnp.int32, (SEQS, DV), 0) % 8
    place = lax.broadcasted_iota(jnp.int32, (SEQS, positions), 1) + kv_index * positions
    scores = []
    for g in range(2):
        s = jnp.zeros((SEQS, positions), F32)
        for b in range(8):
            picked = jnp.where(of_row == b, both[SEQS * g : SEQS * g + SEQS], 0.0).astype(BF16)
            s = s + dot_rows(picked, keys_ref[8 * g + b])
        scores.append(s)
    found = []
    for g, s in enumerate(scores):
        alive = place < limit_ref[SEQS * g : SEQS * g + SEQS, :1]
        s = jnp.where(alive, s * scale_att, MASKED_SCORE)
        top = jnp.max(s, axis=1, keepdims=True)
        e = jnp.where(alive, jnp.exp(s - top), 0.0)
        weights = e.astype(BF16)
        o = jnp.zeros((SEQS, DV), F32)
        for b in range(8):
            o = jnp.where(of_row == b, dot(weights, values_ref[8 * g + b]), o)
        found.append((top, jnp.sum(e, axis=1, keepdims=True), o))
    old, l, o = (jnp.concatenate(pair, axis=0) for pair in zip(*found))
    line = lax.broadcasted_iota(jnp.int32, (rows, 1), 0)
    here = line // SEQS * 8 + line % 8 == kv_index
    own_score = scale_att * jnp.sum(both * key_new, axis=1, keepdims=True)
    own_score = jnp.where(here, own_score, MASKED_SCORE)
    peak = jnp.maximum(old, own_score)
    old_scale = jnp.exp(old - peak)
    fresh = jnp.where(here, jnp.exp(own_score - peak), 0.0)
    l = l * old_scale + fresh
    o = (o * old_scale + fresh * value_new).astype(BF16)
    lane = lane[:8]
    stats = jnp.zeros((8, DV), F32)
    for at, part in zip((0, 32, 64, 96, 112), pieces(peak, 3) + pieces(l, 2)):
        for g in range(4):
            stats = jnp.where(lane == at + g, part[8 * g : 8 * g + 8].astype(F32), stats)
    stats = stats.astype(BF16)
    for j in range(out_ref.shape[0]):
        out_ref[j, :rows, :] = o
        out_ref[j, rows:, :] = stats


def out_products(got_ref, side_ref, gain_ref, w_ref, pack_ref, out_ref):
    count = got_ref.shape[0]
    rows = 2 * SEQS
    stats = [got_ref[j, rows:, :].astype(F32) for j in range(count)]
    peaks = [x + pltpu.roll(x, 96, 1) + pltpu.roll(x, 64, 1) for x in stats]
    sums = [pltpu.roll(x, 32, 1) + pltpu.roll(x, 16, 1) for x in stats]
    peak = functools.reduce(jnp.maximum, peaks)
    scales = [jnp.exp(p - peak) for p in peaks]
    inverse = 1.0 / sum(w * l for w, l in zip(scales, sums))
    mixed = []
    for g in range(4):
        part = sum(
            w[:, g : g + 1] * got_ref[j, 8 * g : 8 * g + 8, :].astype(F32)
            for j, w in enumerate(scales)
        )
        mixed.append(part * inverse[:, g : g + 1])
    head = jnp.concatenate(mixed[::2], axis=0) - side_ref[2] * jnp.concatenate(mixed[1::2], axis=0)
    norm_scale = lax.rsqrt(jnp.mean(head * head, axis=1, keepdims=True) + EPSILON)
    normed = (head * norm_scale * gain_ref[...].astype(F32) * OUTPUT_KEEP).astype(BF16)
    put_copies(out_ref, 0, dot(normed, w_ref[...]).astype(BF16))
    put_copies(out_ref, 128, dot(normed, pack_ref[W_OUT : W_OUT + 128]).astype(BF16))


def last_sum(stream_ref, got_ref, out_ref):
    out_ref[...] = (stream_ref[...].astype(F32) + 0.5 * total(got_ref)).astype(BF16)


def local(
    tokens, lengths, cache_keys, cache_values, lambdas, head_gain, attn_gain, w_query, w_key,
    w_value, w_out, first_gain, first_gate, first_up, first_down, second_gain, second_gate,
    second_up, second_down,
):
    keys = cache_keys.reshape(SEQS, -1, 2 * DK)
    values = cache_values.reshape(SEQS, -1, DV)
    row = lambda g: g.reshape(1, -1)
    shape = jax.ShapeDtypeStruct

    def from_partner(x):
        return lax.ppermute(x, ("kv_a", "kv_b"), PAIR)

    narrow = shape((16, SEQS, 128), BF16)
    double = shape((16, SEQS, 256), BF16)
    stream = shape((SEQS, 128), BF16)

    other_down = from_partner(first_down)
    steps = local_call(rotary_steps, shape((SEQS, 128), F32))
    side, limit = local_call(
        side_tables, (shape((3, SEQS, 128), F32), shape((2 * SEQS, 128), jnp.int32)),
        lambdas, row(lengths), steps, scalars=1, micros=0.01,
    )
    sent = local_call(
        first_products, shape((16, SEQS, 768), BF16),
        tokens, row(first_gain), first_gate.T, first_up.T, side,
    )
    got = exchange(sent, KV)
    hidden, pack = local_call(
        hidden_and_pack, (shape((SEQS, 352), BF16), shape((PACK, 128), BF16)),
        got, w_query, w_key, w_value, second_gate.T, second_up.T, w_out, tokens,
        row(attn_gain), row(second_gain),
    )
    pack = from_partner(pack)
    sent = local_call(down_products_of_pair, double, hidden, first_down, other_down)
    sent, first = local_call(
        head_products, (shape((8, SEQS + 8, 128), BF16), shape((SEQS, 256), BF16)),
        tokens, exchange(sent, "tp"), row(attn_gain), w_query, w_key, w_value, pack,
    )
    sent = local_call(
        attention, shape((16, 2 * SEQS + 8, 128), BF16),
        exchange(sent, HALF), side, limit, keys, values,
    )
    sent = local_call(
        out_products, double, exchange(sent, KV), side, row(head_gain), w_out, pack
    )
    sent, second = local_call(
        second_products, (shape((8, SEQS, 768), BF16), stream),
        first, exchange(sent, "tp"), row(second_gain), second_gate.T, second_up.T, pack,
    )
    sent = local_call(down_products, narrow, exchange(sent, HALF), second_down)
    return local_call(last_sum, stream, second, exchange(sent, "tp"))


def solution(mesh):
    finer = Mesh(mesh.devices.reshape(4, 2, 2, mesh.shape["tp"]), (*KV, "tp"))
    cache = P(None, KV, "tp", None)
    placed = (
        P(None, KV), P(), cache, cache, P("tp"), P(), P(KV), P(KV, "tp"), P(KV, "tp"),
        P(KV, "tp"), P("tp", KV), P(KV), P(KV, "tp"), P(KV, "tp"), P("tp", KV), P(KV),
        P(KV, "tp"), P(KV, "tp"), P("tp", KV),
    )

    return jax.shard_map(local, mesh=finer, in_specs=placed, out_specs=P(None, KV), check_vma=False)
```
